32 devices in a mesh: rep: 2 (over x), fs: 4 (over y, core), tp: 4 (over z).
Axes of the slice: x: 2, y: 2, z: 4, core: 2. Of those that a mesh axis runs over, the one named last changes fastest.
Arguments:
- acts: bfloat16 [2048, 2048], P(('rep', 'fs'), 'tp'), may hold values from -6 to 6
- cotangent: bfloat16 [2048, 2048], P(('rep', 'fs'), 'tp'), may hold values from -8 to 8
- pre_act: bfloat16 [2048, 4096], P(('rep', 'fs'), 'tp'), may hold values from -6 to 6
- up_store: float32 [2048, 4096], P('fs', 'tp'), may hold values from -0.125 to 0.125
- up_scale: float32 [4096], P('tp'), may hold values from 0.5 to 2
- down_store: float32 [4096, 2048], P('tp', 'fs'), may hold values from -0.09375 to 0.09375
- down_scale: float32 [2048], replicated, may hold values from 0.5 to 2
Outputs:
- grad_input: bfloat16 [2048, 2048], P(('rep', 'fs'), 'tp')
- grad_up: float32 [2048, 4096], P('fs', 'tp')
- grad_down: float32 [4096, 2048], P('tp', 'fs')
The draws below stay inside these ranges and needn't reach their ends.
All inputs are finite; a program needn't handle non-finite values.
Results may differ from the reference program's by a relative error of at most 0.007.
Values may be sent and summed in bfloat16 or wider, within the bound.
A program may use at most 128 MiB of HBM per device.

```python
import math
import jax
import jax.numpy as jnp

D = 2048
FF = 4096
TOKENS = 2048


def with_spikes(entries, rng, source, target, blocks, factor):
    owner, partner = [(jnp.arange(entries.shape[dim]) // (entries.shape[dim] // blocks)).reshape([-1 if axis == dim else 1 for axis in range(entries.ndim)]) for dim in (source, target)]
    chosen = jax.random.permutation(rng, blocks)[partner]
    strong = (owner == chosen) | (owner == (partner + blocks // 2) % blocks)
    return jnp.where(strong, factor * entries, entries)


def block_scale(own_key, shape, split, smallest, high):
    gain, own = 1.0, jax.random.fold_in(own_key, 6)
    for axis_at, parts in split:
        draws = jnp.exp(jax.random.uniform(jax.random.fold_in(own, axis_at), (parts,), jnp.float32, smallest / len(split), high / len(split)))
        gain = gain * jnp.repeat(draws, shape[axis_at] // parts).reshape([-1 if axis == axis_at else 1 for axis in range(len(shape))])
    return gain


def noise(stream_key, shape, scale, limit, pieces=(), kind=jnp.bfloat16):
    result = jax.random.normal(stream_key, shape, jnp.float32) * scale
    if len(pieces) > 0:
        result = block_scale(stream_key, shape, pieces, -0.22, 0.18) * result
    return jnp.clip(result, min=-limit, max=limit).astype(kind)


def gaussian_with(key, dims, spread, bound, cuts, heavy, dtype=jnp.bfloat16):
    array = spread * jax.random.normal(key, dims, jnp.float32)
    if cuts:
        array = array * block_scale(key, dims, cuts, -0.22, 0.18)
    return jnp.clip(with_spikes(array, jax.random.fold_in(key, 3), *heavy), -bound, bound).astype(dtype)


def setup_inputs(seed: int = 0) -> dict:
    arg_keys = jax.random.split(jax.random.key(seed), 8)
    return {
        "acts": noise(arg_keys[0], (TOKENS, D), 1.0, 6.0, ((0, 8), (1, 4))),
        "cotangent": gaussian_with(arg_keys[1], (TOKENS, D), 1.0, 8.0, ((0, 8), (1, 4)), (0, 1, 8, 2.0)),
        "pre_act": noise(arg_keys[2], (TOKENS, FF), 1.0, 6.0, ((0, 8), (1, 4))),
        "up_store": noise(arg_keys[3], (D, FF), D ** -0.5, 0.125, ((0, 4), (1, 4)), jnp.float32),
        "up_scale": jnp.clip(jnp.exp(math.log(2.0) - 1.3862944 * jax.random.uniform(arg_keys[4], (FF,), jnp.float32) ** block_scale(arg_keys[4], (FF,), ((0, 4),), -0.2, 0.2)), 0.5, 2.0),
        "down_store": noise(arg_keys[5], (FF, D), FF ** -0.5, 0.09375, ((0, 4), (1, 4)), jnp.float32),
        "down_scale": jnp.clip(jnp.exp(jax.random.uniform(arg_keys[6], (D,), jnp.float32, math.log(0.5), math.log(2.0))), 0.5, 2.0),
    }


def reference(acts, cotangent, pre_act, up_store, up_scale, down_store, down_scale):
    norm_factor = 1.0 / math.sqrt(TOKENS)
    scaled = (cotangent.astype(jnp.float32) * down_scale[None, :]).astype(jnp.bfloat16)
    d_act = jnp.dot(scaled, down_store.astype(jnp.bfloat16).T, preferred_element_type=jnp.float32)
    positive = jnp.maximum(pre_act.astype(jnp.float32), 0.0)
    act = (positive * positive).astype(jnp.bfloat16)
    d_pre = (2.0 * positive * d_act * up_scale[None, :]).astype(jnp.bfloat16)
    grad_down = jnp.dot(act.T, scaled, preferred_element_type=jnp.float32) * norm_factor
    grad_up = jnp.dot(acts.T, d_pre, preferred_element_type=jnp.float32) * norm_factor
    grad_input = jnp.dot(d_pre, up_store.astype(jnp.bfloat16).T, preferred_element_type=jnp.float32).astype(jnp.bfloat16)
    return (grad_input, grad_up, grad_down)
```

```python
import functools
import math

import jax
import jax.numpy as jnp
from jax import lax
from jax.experimental import pallas as pl
from jax.experimental.pallas import tpu as pltpu
from jax.sharding import PartitionSpec as P

F32, BF16 = jnp.float32, jnp.bfloat16


def dot(left, right, dims):
    return lax.dot_general(left, right, (dims, ((), ())), preferred_element_type=F32)


def fitting(size, most):
    return most if size % most == 0 else size


def kernel(
    sizes,
    acts, cotangent, pre_act, up_store, up_scale, down_store, down_scale,
    grad_input, grad_up, grad_down,
    blocks, scaled_cols, acts_cols, act_group, dpre_group, down_bf, up_bf,
    pair_out, pair_in, far_out, far_in, d_act, gi_out, gi_in,
    gd_out, gd_in, gu_out, gu_in,
    z_send, z_recv, col_send, col_recv, act_send, act_recv, dpre_send, dpre_recv,
    pair_send, pair_recv, far_send, far_recv, gi_send, gi_recv,
    gd_send, gd_recv, gu_send, gu_recv,
):
    reps, F, T = sizes
    n, d = acts.shape
    h = pre_act.shape[1]
    w = down_store.shape[1]
    half, sub = F // 2, F // T
    norm_factor = 1.0 / math.sqrt(n * F * reps)
    r, f, z = lax.axis_index("rep"), lax.axis_index("fs"), lax.axis_index("tp")
    core, place = lax.rem(f, 2), lax.div(f, 2)
    partner = f + 1 - 2 * core

    def rows(at):
        return pl.ds(pl.multiple_of(at * n, n), n)

    def remote(src, dst, send, recv, where):
        return pltpu.make_async_remote_copy(
            src_ref=src, dst_ref=dst, send_sem=send, recv_sem=recv,
            device_id=where, device_id_type=pl.DeviceIdType.MESH,
        )

    def landed(ref, recv):
        remote(ref, ref, recv, recv, {"fs": partner}).wait_recv()

    def left_for(ref, send):
        remote(ref, ref, send, send, {"fs": partner}).wait_send()

    cols = (scaled_cols, acts_cols)

    def pass_on(a, block, way):
        @pl.when((z < T - 1) if way == 0 else (z > 0))
        def _():
            ref = blocks.at[a, block]
            to = z + 1 if way == 0 else z - 1
            remote(ref, ref, z_send.at[a, block, way], z_recv.at[a, block], {"tp": to}).start()

    def spread(a, block):
        for j in range(sub):
            target = block * sub + j

            @pl.when(target != f)
            def _():
                remote(
                    blocks.at[a, block, :, pl.ds(j * w, w)], cols[a].at[rows(f)],
                    col_send.at[a, target], col_recv.at[a, f], {"fs": target},
                ).start()

            @pl.when(target == f)
            def _():
                cols[a][rows(f), :] = blocks[a, block, :, j * w:(j + 1) * w]

    def own_block(a):
        pass_on(a, z, 0)
        pass_on(a, z, 1)
        spread(a, z)

    def arriving(a, s):
        @pl.when(z - s >= 0)
        def _():
            landed(blocks.at[a, z - s], z_recv.at[a, z - s])
            pass_on(a, z - s, 0)
            spread(a, z - s)

        @pl.when(z + s <= T - 1)
        def _():
            landed(blocks.at[a, z + s], z_recv.at[a, z + s])
            pass_on(a, z + s, 1)
            spread(a, z + s)

    def cols_landed(a, source):
        @pl.when(source != f)
        def _():
            landed(cols[a].at[rows(source)], col_recv.at[a, source])

    def group_start(group, send, recv):
        ref = group.at[rows(f)]
        for k in range(1, half):
            to = lax.rem(f + 2 * k, F)
            remote(ref, ref, send.at[k], recv.at[f], {"fs": to}).start()
        remote(ref, ref, send.at[0], recv.at[f], {"fs": partner}).start()

    def group_forward(group, send, recv, k):
        source = lax.rem(f - 2 * k + F, F)
        ref = group.at[rows(source)]
        landed(ref, recv.at[source])
        remote(ref, ref, send.at[half - 1 + k], recv.at[source], {"fs": partner}).start()
        return source

    def group_sent(group, send):
        for k in range(F - 1):
            left_for(group.at[rows(f)], send.at[k])

    scale = down_scale[:, pl.ds(pl.multiple_of(z * d, d), d)]
    blocks[0, z] = (cotangent[...].astype(F32) * scale).astype(BF16)
    own_block(0)
    positive = jnp.maximum(pre_act[...].astype(F32), 0.0)
    act_group[rows(f), :] = (positive * positive).astype(BF16)
    group_start(act_group, act_send, act_recv)
    blocks[1, z] = acts[...]
    down_bf[...] = down_store[...].astype(BF16)
    for s in range(1, T):
        arriving(0, s)
    own_block(1)
    up_bf[...] = up_store[...].astype(BF16)

    def partial_of(target):
        cols_landed(0, target)
        return dot(scaled_cols[rows(target), :], down_bf[...], ((1,), (1,)))

    def for_partner(k, carry):
        i = lax.rem(place + k, half)
        pair_out[i] = partial_of(2 * i + 1 - core).astype(BF16)
        remote(
            pair_out.at[i], pair_in.at[i], pair_send.at[i], pair_recv.at[i], {"fs": partner}
        ).start()
        return carry

    lax.fori_loop(1, half + 1, for_partner, 0)

    def for_far(k, carry):
        i = lax.rem(place + k, half)
        value = partial_of(2 * i + core)
        landed(pair_in.at[i], pair_recv.at[i])
        far_out[i] = (value + pair_in[i].astype(F32)).astype(BF16)
        remote(
            far_out.at[i], far_in.at[place], far_send.at[i], far_recv.at[place],
            {"fs": 2 * i + core},
        ).start()
        return carry

    lax.fori_loop(1, half, for_far, 0)
    value = partial_of(f)
    landed(pair_in.at[place], pair_recv.at[place])
    d_act[...] = value + pair_in[place].astype(F32)

    for k in range(1, half):
        group_forward(act_group, act_send, act_recv, k)
    for s in range(1, T):
        arriving(1, s)

    landed(act_group.at[rows(partner)], act_recv.at[partner])
    for k in range(1, half):
        source = lax.rem(partner + 2 * k, F)
        landed(act_group.at[rows(source)], act_recv.at[source])
    gd_rows = gd_out.shape[1]

    def rep_copy(out, into, send, recv, c, p):
        to = lax.rem(r + p, reps)
        return remote(
            out.at[c], into.at[p - 1, c], send.at[p - 1, c], recv.at[p - 1, c], {"rep": to}
        )

    def down_step(c, carry):
        at = pl.ds(pl.multiple_of(c * gd_rows, gd_rows), gd_rows)
        value = dot(act_group[:, at], scaled_cols[...], ((0,), (0,))) * norm_factor
        gd_out[c] = value.astype(BF16)
        for p in range(1, reps):
            rep_copy(gd_out, gd_in, gd_send, gd_recv, c, p).start()
        return carry

    lax.fori_loop(0, gd_out.shape[0], down_step, 0)

    total = d_act[...]
    for k in range(1, half):
        j = lax.rem(place + k, half)
        landed(far_in.at[j], far_recv.at[j])
        total = total + far_in[j].astype(F32)
    positive = jnp.maximum(pre_act[...].astype(F32), 0.0)
    dpre_group[rows(f), :] = (2.0 * positive * total * up_scale[...]).astype(BF16)
    group_start(dpre_group, dpre_send, dpre_recv)

    home = lax.div(f, sub)
    slot = z * sub + lax.rem(f, sub)

    def input_part(source):
        gi_out[source] = dot(dpre_group[rows(source), :], up_bf[...], ((1,), (1,))).astype(BF16)

        @pl.when((source != f) | (home != z))
        def _():
            remote(
                gi_out.at[source], gi_in.at[slot], gi_send.at[source], gi_recv.at[slot],
                {"fs": source, "tp": home},
            ).start()

        @pl.when((source == f) & (home == z))
        def _():
            gi_in[slot] = gi_out[source]

    input_part(f)
    for k in range(1, half):
        input_part(group_forward(dpre_group, dpre_send, dpre_recv, k))
    landed(dpre_group.at[rows(partner)], dpre_recv.at[partner])
    input_part(partner)
    for k in range(1, half):
        source = lax.rem(partner + 2 * k, F)
        landed(dpre_group.at[rows(source)], dpre_recv.at[source])
        input_part(source)

    for source in range(F):
        cols_landed(1, source)
    gu_rows = gu_out.shape[1]
    for c in range(gu_out.shape[0]):
        value = dot(acts_cols[:, c * gu_rows:(c + 1) * gu_rows], dpre_group[...], ((0,), (0,)))
        gu_out[c] = (value * norm_factor).astype(BF16)
        for p in range(1, reps):
            rep_copy(gu_out, gu_in, gu_send, gu_recv, c, p).start()

    def finish(out, into, send, recv, result):
        step_rows = out.shape[1]

        def step(c, carry):
            for p in range(1, reps):
                rep_copy(out, into, send, recv, c, p).wait()
            value = out[c].astype(F32)
            for p in range(1, reps):
                value = value + into[p - 1, c].astype(F32)
            result[pl.ds(pl.multiple_of(c * step_rows, step_rows), step_rows), :] = value
            return carry

        lax.fori_loop(0, out.shape[0], step, 0)

    finish(gd_out, gd_in, gd_send, gd_recv, grad_down)
    for j in range(sub):
        value = jnp.zeros((n, w), F32)
        for s in range(T):
            at = s * sub + j

            @pl.when((s != z) | (z * sub + j != f))
            def _():
                landed(gi_in.at[at], gi_recv.at[at])

            value = value + gi_in[at].astype(F32)
        grad_input[:, j * w:(j + 1) * w] = value.astype(BF16)
    finish(gu_out, gu_in, gu_send, gu_recv, grad_up)

    for a in range(2):
        for block in range(T):
            @pl.when((block <= z) & (z < T - 1))
            def _():
                left_for(blocks.at[a, block], z_send.at[a, block, 0])

            @pl.when((block >= z) & (z > 0))
            def _():
                left_for(blocks.at[a, block], z_send.at[a, block, 1])

        for target in range(F):
            @pl.when(target != f)
            def _():
                left_for(cols[a].at[rows(f)], col_send.at[a, target])
    group_sent(act_group, act_send)
    group_sent(dpre_group, dpre_send)
    for i in range(half):
        left_for(pair_out.at[i], pair_send.at[i])

        @pl.when(i != place)
        def _():
            left_for(far_out.at[i], far_send.at[i])
    for source in range(F):
        @pl.when((source != f) | (home != z))
        def _():
            left_for(gi_out.at[source], gi_send.at[source])


def body(sizes, acts, cotangent, pre_act, up_store, up_scale, down_store, down_scale):
    reps, F, T = sizes
    n, d = acts.shape
    h = pre_act.shape[1]
    w = down_store.shape[1]
    half, sub = F // 2, F // T
    gd_rows, gu_rows = fitting(h, 256), fitting(w, 256)
    gd_steps, gu_steps = h // gd_rows, w // gu_rows
    others = max(reps - 1, 1)
    sem = pltpu.SemaphoreType.DMA
    vmem = pl.BlockSpec(memory_space=pltpu.VMEM)
    return pl.pallas_call(
        functools.partial(kernel, sizes),
        out_shape=(
            jax.ShapeDtypeStruct((n, d), BF16),
            jax.ShapeDtypeStruct((w, h), F32),
            jax.ShapeDtypeStruct((h, w), F32),
        ),
        in_specs=[vmem] * 7,
        out_specs=(vmem, vmem, vmem),
        scratch_shapes=[
            pltpu.VMEM((2, T, n, d), BF16),
            pltpu.VMEM((F * n, w), BF16),
            pltpu.VMEM((F * n, w), BF16),
            pltpu.VMEM((F * n, h), BF16),
            pltpu.VMEM((F * n, h), BF16),
            pltpu.VMEM((h, w), BF16),
            pltpu.VMEM((w, h), BF16),
            pltpu.VMEM((half, n, h), BF16),
            pltpu.VMEM((half, n, h), BF16),
            pltpu.VMEM((half, n, h), BF16),
            pltpu.VMEM((half, n, h), BF16),
            pltpu.VMEM((n, h), F32),
            pltpu.VMEM((F, n, w), BF16),
            pltpu.VMEM((F, n, w), BF16),
            pltpu.VMEM((gd_steps, gd_rows, w), BF16),
            pltpu.VMEM((others, gd_steps, gd_rows, w), BF16),
            pltpu.VMEM((gu_steps, gu_rows, h), BF16),
            pltpu.VMEM((others, gu_steps, gu_rows, h), BF16),
            sem((2, T, 2)), sem((2, T)), sem((2, F)), sem((2, F)),
            sem((F,)), sem((F,)), sem((F,)), sem((F,)),
            sem((half,)), sem((half,)), sem((half,)), sem((half,)),
            sem((F,)), sem((F,)),
            sem((others, gd_steps)), sem((others, gd_steps)),
            sem((others, gu_steps)), sem((others, gu_steps)),
        ],
        compiler_params=pltpu.CompilerParams(
            has_side_effects=True, vmem_limit_bytes=60 * 1024 * 1024
        ),
    )(
        acts, cotangent, pre_act, up_store, up_scale.reshape(1, h), down_store,
        down_scale.reshape(1, d * T),
    )


def solution(mesh):
    sizes = (mesh.shape["rep"], mesh.shape["fs"], mesh.shape["tp"])
    return jax.shard_map(
        functools.partial(body, sizes),
        mesh=mesh,
        in_specs=(
            P(("rep", "fs"), "tp"),
            P(("rep", "fs"), "tp"),
            P(("rep", "fs"), "tp"),
            P("fs", "tp"),
            P("tp"),
            P("tp", "fs"),
            P(),
        ),
        out_specs=(P(("rep", "fs"), "tp"), P("fs", "tp"), P("tp", "fs")),
        check_vma=False,
    )
```

```python
import functools
import math

import jax
import jax.numpy as jnp
from jax import lax
from jax.experimental import pallas as pl
from jax.experimental.pallas import tpu as pltpu
from jax.sharding import PartitionSpec as P

F32, BF16 = jnp.float32, jnp.bfloat16


def dot(left, right, dims):
    return lax.dot_general(left, right, (dims, ((), ())), preferred_element_type=F32)


def fitting(size, most):
    return most if size % most == 0 else size


def kernel(
    sizes,
    acts, cotangent, pre_act, up_store, up_scale, down_store, down_scale,
    grad_input, grad_up, grad_down,
    up_f32, down_f32,
    blocks, scaled_cols, acts_cols, act_group, dpre_group, down_bf, up_bf,
    pair_out, pair_in, far_out, far_in, d_act, gi_out, gi_in,
    gd_out, gd_in, gu_out, gu_in,
    load_sem,
    z_send, z_recv, col_send, col_recv, act_send, act_recv, dpre_send, dpre_recv,
    pair_send, pair_recv, far_send, far_recv, gi_send, gi_recv,
    gd_send, gd_recv, gu_send, gu_recv,
):
    reps, F, T = sizes
    n, d = acts.shape
    h = pre_act.shape[1]
    w = down_store.shape[1]
    half, sub = F // 2, F // T
    chunks, cw = blocks.shape[2], blocks.shape[4]
    per = w // cw
    parts, hp = dpre_group.shape[0], dpre_group.shape[2]
    norm_factor = 1.0 / math.sqrt(n * F * reps)
    r, f, z = lax.axis_index("rep"), lax.axis_index("fs"), lax.axis_index("tp")
    core, place = lax.rem(f, 2), lax.div(f, 2)
    partner = f + 1 - 2 * core
    mesh_ids = pl.DeviceIdType.MESH

    down_load = pltpu.make_async_copy(down_store, down_f32, load_sem.at[0])
    up_load = pltpu.make_async_copy(up_store, up_f32, load_sem.at[1])
    down_load.start()
    up_load.start()

    barrier = pltpu.get_barrier_semaphore()

    def greet(at, carry):
        to_f, to_z = lax.div(at, T), lax.rem(at, T)

        @pl.when((to_f != f) | (to_z != z))
        def _():
            pl.semaphore_signal(
                barrier, inc=1, device_id={"fs": to_f, "tp": to_z}, device_id_type=mesh_ids
            )

        return carry

    lax.fori_loop(0, F * T, greet, 0)
    for p in range(1, reps):
        pl.semaphore_signal(
            barrier, inc=1, device_id={"rep": lax.rem(r + p, reps)}, device_id_type=mesh_ids
        )

    def rows(at):
        return pl.ds(pl.multiple_of(at * n, n), n)

    def remote(src, dst, send, recv, where):
        return pltpu.make_async_remote_copy(
            src_ref=src, dst_ref=dst, send_sem=send, recv_sem=recv,
            device_id=where, device_id_type=mesh_ids,
        )

    def landed(ref, recv):
        remote(ref, ref, recv, recv, {"fs": partner}).wait_recv()

    def left_for(ref, send):
        remote(ref, ref, send, send, {"fs": partner}).wait_send()

    cols = (scaled_cols, acts_cols)

    def pass_on(a, block, g, way):
        @pl.when((z < T - 1) if way == 0 else (z > 0))
        def _():
            ref = blocks.at[a, block, g]
            to = z + 1 if way == 0 else z - 1
            remote(ref, ref, z_send.at[a, block, g, way], z_recv.at[a, block, g], {"tp": to}).start()

    def spread(a, block, g):
        target, q = block * sub + g // per, g % per

        @pl.when(target != f)
        def _():
            remote(
                blocks.at[a, block, g], cols[a].at[q, rows(f)],
                col_send.at[a, block, g], col_recv.at[a, f, q], {"fs": target},
            ).start()

        @pl.when(target == f)
        def _():
            cols[a][q, rows(f), :] = blocks[a, block, g]

    def own_block(a):
        for g in range(chunks):
            pass_on(a, z, g, 0)
            pass_on(a, z, g, 1)
        for g in range(chunks):
            spread(a, z, g)

    def arriving(a, s):
        for g in range(chunks):
            @pl.when(z - s >= 0)
            def _():
                landed(blocks.at[a, z - s, g], z_recv.at[a, z - s, g])
                pass_on(a, z - s, g, 0)
                spread(a, z - s, g)

            @pl.when(z + s <= T - 1)
            def _():
                landed(blocks.at[a, z + s, g], z_recv.at[a, z + s, g])
                pass_on(a, z + s, g, 1)
                spread(a, z + s, g)

    def cols_landed(a, source):
        @pl.when(source != f)
        def _():
            for q in range(per):
                landed(cols[a].at[q, rows(source)], col_recv.at[a, source, q])

    def group_start(group, send, recv):
        ref = group.at[rows(f)]
        for k in range(1, half):
            to = lax.rem(f + 2 * k, F)
            remote(ref, ref, send.at[k], recv.at[f], {"fs": to}).start()
        remote(ref, ref, send.at[0], recv.at[f], {"fs": partner}).start()

    def group_forward(group, send, recv):
        for k in range(1, half):
            source = lax.rem(f - 2 * k + F, F)
            ref = group.at[rows(source)]
            landed(ref, recv.at[source])
            remote(ref, ref, send.at[half - 1 + k], recv.at[source], {"fs": partner}).start()

    def forwards_landed(group, recv):
        for k in range(1, half):
            source = lax.rem(partner + 2 * k, F)
            landed(group.at[rows(source)], recv.at[source])

    def group_sent(group, send):
        for k in range(F - 1):
            left_for(group.at[rows(f)], send.at[k])

    scale = down_scale[:, pl.ds(pl.multiple_of(z * d, d), d)]
    scaled = (cotangent[...].astype(F32) * scale).astype(BF16)
    for g in range(chunks):
        blocks[0, z, g] = scaled[:, g * cw:(g + 1) * cw]
    positive = jnp.maximum(pre_act[...].astype(F32), 0.0)
    act_group[rows(f), :] = (positive * positive).astype(BF16)
    pl.semaphore_wait(barrier, F * T - 1 + reps - 1)
    own_block(0)
    group_start(act_group, act_send, act_recv)
    for g in range(chunks):
        blocks[1, z, g] = acts[:, g * cw:(g + 1) * cw]
    down_load.wait()
    down_bf[...] = down_f32[...].astype(BF16)
    for s in range(1, T):
        if s == T - 1:
            group_forward(act_group, act_send, act_recv)
        arriving(0, s)
    own_block(1)

    def partial_of(target, e):
        value = jnp.zeros((n, hp), F32)
        for q in range(per):
            value = value + dot(
                scaled_cols[q, rows(target), :],
                down_bf[e * hp:(e + 1) * hp, q * cw:(q + 1) * cw], ((1,), (1,)),
            )
        return value

    for e in range(parts):
        def for_partner(k, carry):
            i = lax.rem(place + k, half)
            if e == 0:
                cols_landed(0, 2 * i + 1 - core)
            pair_out[e, i] = partial_of(2 * i + 1 - core, e).astype(BF16)
            remote(
                pair_out.at[e, i], pair_in.at[e, i], pair_send.at[e, i], pair_recv.at[e, i],
                {"fs": partner},
            ).start()
            return carry

        lax.fori_loop(1, half + 1, for_partner, 0)
    for e in range(parts):
        def for_far(k, carry):
            i = lax.rem(place + k, half)
            if e == 0:
                cols_landed(0, 2 * i + core)
            value = partial_of(2 * i + core, e)
            landed(pair_in.at[e, i], pair_recv.at[e, i])
            far_out[e, i] = (value + pair_in[e, i].astype(F32)).astype(BF16)
            remote(
                far_out.at[e, i], far_in.at[e, place], far_send.at[e, i], far_recv.at[e, place],
                {"fs": 2 * i + core},
            ).start()
            return carry

        lax.fori_loop(1, half, for_far, 0)
    for e in range(parts):
        value = partial_of(f, e)
        landed(pair_in.at[e, place], pair_recv.at[e, place])
        d_act[e] = value + pair_in[e, place].astype(F32)

    landed(act_group.at[rows(partner)], act_recv.at[partner])
    forwards_landed(act_group, act_recv)
    gd_rows = gd_out.shape[1]

    def rep_copy(out, into, send, recv, c, p):
        to = lax.rem(r + p, reps)
        return remote(
            out.at[c], into.at[p - 1, c], send.at[p - 1, c], recv.at[p - 1, c], {"rep": to}
        )

    def down_step(c, carry):
        at = pl.ds(pl.multiple_of(c * gd_rows, gd_rows), gd_rows)
        for q in range(per):
            value = dot(act_group[:, at], scaled_cols[q], ((0,), (0,))) * norm_factor
            gd_out[c, :, q * cw:(q + 1) * cw] = value.astype(BF16)
        for p in range(1, reps):
            rep_copy(gd_out, gd_in, gd_send, gd_recv, c, p).start()
        return carry

    lax.fori_loop(0, gd_out.shape[0], down_step, 0)
    arriving(1, 1)
    for e in range(parts):
        total = d_act[e]
        for k in range(1, half):
            j = lax.rem(place + k, half)
            landed(far_in.at[e, j], far_recv.at[e, j])
            total = total + far_in[e, j].astype(F32)
        at = slice(e * hp, (e + 1) * hp)
        positive = jnp.maximum(pre_act[:, at].astype(F32), 0.0)
        dpre_group[e, rows(f), :] = (2.0 * positive * total * up_scale[:, at]).astype(BF16)
        group_start(dpre_group.at[e], dpre_send.at[e], dpre_recv.at[e])
        if e == 0:
            up_load.wait()
            up_bf[...] = up_f32[...].astype(BF16)
            for s in range(2, T - 1):
                arriving(1, s)
    if T > 2:
        arriving(1, T - 1)

    home = lax.div(f, sub)
    slot = z * sub + lax.rem(f, sub)

    def input_part(source):
        value = jnp.zeros((n, w), F32)
        for e in range(parts):
            value = value + dot(
                dpre_group[e, rows(source), :], up_bf[:, e * hp:(e + 1) * hp], ((1,), (1,))
            )
        gi_out[source] = value.astype(BF16)

        @pl.when((source != f) | (home != z))
        def _():
            remote(
                gi_out.at[source], gi_in.at[slot], gi_send.at[source], gi_recv.at[slot],
                {"fs": source, "tp": home},
            ).start()

        @pl.when((source == f) & (home == z))
        def _():
            gi_in[slot] = gi_out[source]

    input_part(f)
    for e in range(parts):
        group_forward(dpre_group.at[e], dpre_send.at[e], dpre_recv.at[e])
        landed(dpre_group.at[e, rows(partner)], dpre_recv.at[e, partner])
        forwards_landed(dpre_group.at[e], dpre_recv.at[e])
        if e == 0:
            for source in range(F):
                cols_landed(1, source)
        for q in range(per):
            value = dot(acts_cols[q], dpre_group[e], ((0,), (0,)))
            gu_out[e, q * cw:(q + 1) * cw, :] = (value * norm_factor).astype(BF16)
        for p in range(1, reps):
            rep_copy(gu_out, gu_in, gu_send, gu_recv, e, p).start()
    for k in range(1, half):
        input_part(lax.rem(f + 2 * k, F))
        input_part(lax.rem(partner + 2 * k, F))
    input_part(partner)

    def total_of(out, into, send, recv, c):
        for p in range(1, reps):
            rep_copy(out, into, send, recv, c, p).wait()
        value = out[c].astype(F32)
        for p in range(1, reps):
            value = value + into[p - 1, c].astype(F32)
        return value

    def finish_down(c, carry):
        at = pl.ds(pl.multiple_of(c * gd_rows, gd_rows), gd_rows)
        grad_down[at, :] = total_of(gd_out, gd_in, gd_send, gd_recv, c)
        return carry

    lax.fori_loop(0, gd_out.shape[0], finish_down, 0)
    for e in range(parts - 1):
        grad_up[:, e * hp:(e + 1) * hp] = total_of(gu_out, gu_in, gu_send, gu_recv, e)
    for j in range(sub):
        value = jnp.zeros((n, w), F32)
        for s in range(T):
            at = s * sub + j

            @pl.when((s != z) | (z * sub + j != f))
            def _():
                landed(gi_in.at[at], gi_recv.at[at])

            value = value + gi_in[at].astype(F32)
        grad_input[:, j * w:(j + 1) * w] = value.astype(BF16)
    grad_up[:, (parts - 1) * hp:] = total_of(gu_out, gu_in, gu_send, gu_recv, parts - 1)

    for a in range(2):
        for block in range(T):
            for g in range(chunks):
                @pl.when((block <= z) & (z < T - 1))
                def _():
                    left_for(blocks.at[a, block, g], z_send.at[a, block, g, 0])

                @pl.when((block >= z) & (z > 0))
                def _():
                    left_for(blocks.at[a, block, g], z_send.at[a, block, g, 1])

                @pl.when(block * sub + g // per != f)
                def _():
                    left_for(blocks.at[a, block, g], col_send.at[a, block, g])
    group_sent(act_group, act_send)
    for e in range(parts):
        group_sent(dpre_group.at[e], dpre_send.at[e])
        for i in range(half):
            left_for(pair_out.at[e, i], pair_send.at[e, i])

            @pl.when(i != place)
            def _():
                left_for(far_out.at[e, i], far_send.at[e, i])
    for source in range(F):
        @pl.when((source != f) | (home != z))
        def _():
            left_for(gi_out.at[source], gi_send.at[source])


def body(sizes, acts, cotangent, pre_act, up_store, up_scale, down_store, down_scale):
    reps, F, T = sizes
    n, d = acts.shape
    h = pre_act.shape[1]
    w = down_store.shape[1]
    half = F // 2
    cw = w // 2 if w % 256 == 0 else w
    per, chunks = w // cw, d // cw
    parts = 2 if h % 256 == 0 else 1
    hp = h // parts
    gd_rows = fitting(h, 256)
    gd_steps = h // gd_rows
    others = max(reps - 1, 1)
    sem = pltpu.SemaphoreType.DMA
    vmem, anywhere = (pl.BlockSpec(memory_space=s) for s in (pltpu.VMEM, pltpu.HBM))
    arrays = [
        ((w, h), F32), ((h, w), F32),
        ((2, T, chunks, n, cw), BF16),
        ((per, F * n, cw), BF16), ((per, F * n, cw), BF16),
        ((F * n, h), BF16), ((parts, F * n, hp), BF16),
        ((h, w), BF16), ((w, h), BF16),
        ((parts, half, n, hp), BF16), ((parts, half, n, hp), BF16),
        ((parts, half, n, hp), BF16), ((parts, half, n, hp), BF16),
        ((parts, n, hp), F32),
        ((F, n, w), BF16), ((F, n, w), BF16),
        ((gd_steps, gd_rows, w), BF16), ((others, gd_steps, gd_rows, w), BF16),
        ((parts, w, hp), BF16), ((others, parts, w, hp), BF16),
    ]
    held = sum(math.prod(shape) * jnp.dtype(kind).itemsize for shape, kind in arrays)
    held += 2 * w * h * 4 + 2 * (3 * n * d + n * h)
    return pl.pallas_call(
        functools.partial(kernel, sizes),
        out_shape=(
            jax.ShapeDtypeStruct((n, d), BF16),
            jax.ShapeDtypeStruct((w, h), F32),
            jax.ShapeDtypeStruct((h, w), F32),
        ),
        in_specs=[vmem, vmem, vmem, anywhere, vmem, anywhere, vmem],
        out_specs=(vmem, vmem, vmem),
        scratch_shapes=[pltpu.VMEM(shape, kind) for shape, kind in arrays] + [
            sem((2,)),
            sem((2, T, chunks, 2)), sem((2, T, chunks)), sem((2, T, chunks)), sem((2, F, per)),
            sem((F,)), sem((F,)), sem((parts, F)), sem((parts, F)),
            sem((parts, half)), sem((parts, half)), sem((parts, half)), sem((parts, half)),
            sem((F,)), sem((F,)),
            sem((others, gd_steps)), sem((others, gd_steps)),
            sem((others, parts)), sem((others, parts)),
        ],
        compiler_params=pltpu.CompilerParams(
            collective_id=0, has_side_effects=True,
            vmem_limit_bytes=min(held + 10 * 1024 * 1024, 60 * 1024 * 1024),
        ),
    )(
        acts, cotangent, pre_act, up_store, up_scale.reshape(1, h), down_store,
        down_scale.reshape(1, d * T),
    )


def solution(mesh):
    sizes = (mesh.shape["rep"], mesh.shape["fs"], mesh.shape["tp"])
    return jax.shard_map(
        functools.partial(body, sizes),
        mesh=mesh,
        in_specs=(
            P(("rep", "fs"), "tp"),
            P(("rep", "fs"), "tp"),
            P(("rep", "fs"), "tp"),
            P("fs", "tp"),
            P("tp"),
            P("tp", "fs"),
            P(),
        ),
        out_specs=(P(("rep", "fs"), "tp"), P("fs", "tp"), P("tp", "fs")),
        check_vma=False,
    )
```

```python
import functools
import math

import jax
import jax.numpy as jnp
from jax import lax
from jax.experimental import pallas as pl
from jax.experimental.pallas import tpu as pltpu
from jax.sharding import PartitionSpec as P

F32, BF16 = jnp.float32, jnp.bfloat16


def dot(left, right, dims):
    return lax.dot_general(left, right, (dims, ((), ())), preferred_element_type=F32)


def fitting(size, most):
    return most if size % most == 0 else size


def kernel(
    sizes,
    acts, cotangent, pre_act, up_store, up_scale, down_store, down_scale,
    grad_input, grad_up, grad_down,
    up_f32, down_f32,
    blocks, scaled_cols, acts_cols, act_group, dpre_group, down_bf, up_bf,
    pair_out, pair_in, far_out, far_in, d_act, gi_out, gi_mid, gi_in,
    gd_out, gd_in, gu_out, gu_in,
    load_sem,
    z_send, z_recv, col_send, col_recv, act_send, act_recv, dpre_send, dpre_recv,
    pair_send, pair_recv, far_send, far_recv, mid_send, mid_recv, gi_send, gi_recv,
    gd_send, gd_recv, gu_send, gu_recv,
):
    reps, F, T = sizes
    n, d = acts.shape
    h = pre_act.shape[1]
    w = down_store.shape[1]
    half, sub = F // 2, F // T
    chunks, cw = blocks.shape[2], blocks.shape[4]
    per = w // cw
    parts, hp = dpre_group.shape[0], dpre_group.shape[2]
    norm_factor = 1.0 / math.sqrt(n * F * reps)
    r, f, z = lax.axis_index("rep"), lax.axis_index("fs"), lax.axis_index("tp")
    core, place = lax.rem(f, 2), lax.div(f, 2)
    partner = f + 1 - 2 * core
    mesh_ids = pl.DeviceIdType.MESH

    down_load = pltpu.make_async_copy(down_store, down_f32, load_sem.at[0])
    up_load = pltpu.make_async_copy(up_store, up_f32, load_sem.at[1])
    down_load.start()
    up_load.start()

    barrier = pltpu.get_barrier_semaphore()

    def greet(at, carry):
        to_f, to_z = lax.div(at, T), lax.rem(at, T)

        @pl.when((to_f != f) | (to_z != z))
        def _():
            pl.semaphore_signal(
                barrier, inc=1, device_id={"fs": to_f, "tp": to_z}, device_id_type=mesh_ids
            )

        return carry

    lax.fori_loop(0, F * T, greet, 0)
    for p in range(1, reps):
        pl.semaphore_signal(
            barrier, inc=1, device_id={"rep": lax.rem(r + p, reps)}, device_id_type=mesh_ids
        )

    def rows(at):
        return pl.ds(pl.multiple_of(at * n, n), n)

    def remote(src, dst, send, recv, where):
        return pltpu.make_async_remote_copy(
            src_ref=src, dst_ref=dst, send_sem=send, recv_sem=recv,
            device_id=where, device_id_type=mesh_ids,
        )

    def landed(ref, recv):
        remote(ref, ref, recv, recv, {"fs": partner}).wait_recv()

    def left_for(ref, send):
        remote(ref, ref, send, send, {"fs": partner}).wait_send()

    cols = (scaled_cols, acts_cols)

    def pass_on(a, block, g, way):
        @pl.when((z < T - 1) if way == 0 else (z > 0))
        def _():
            ref = blocks.at[a, block, g]
            to = z + 1 if way == 0 else z - 1
            remote(ref, ref, z_send.at[a, block, g, way], z_recv.at[a, block, g], {"tp": to}).start()

    def spread(a, block, g):
        target, q = block * sub + g // per, g % per

        @pl.when(target != f)
        def _():
            remote(
                blocks.at[a, block, g], cols[a].at[q, rows(f)],
                col_send.at[a, block, g], col_recv.at[a, f, q], {"fs": target},
            ).start()

        @pl.when(target == f)
        def _():
            cols[a][q, rows(f), :] = blocks[a, block, g]

    def own_block(a):
        for g in range(chunks):
            pass_on(a, z, g, 0)
            pass_on(a, z, g, 1)
        for g in range(chunks):
            spread(a, z, g)

    def arriving(a, s):
        for g in range(chunks):
            @pl.when(z - s >= 0)
            def _():
                landed(blocks.at[a, z - s, g], z_recv.at[a, z - s, g])
                pass_on(a, z - s, g, 0)
                spread(a, z - s, g)

            @pl.when(z + s <= T - 1)
            def _():
                landed(blocks.at[a, z + s, g], z_recv.at[a, z + s, g])
                pass_on(a, z + s, g, 1)
                spread(a, z + s, g)

    def cols_landed(a, source):
        @pl.when(source != f)
        def _():
            for q in range(per):
                landed(cols[a].at[q, rows(source)], col_recv.at[a, source, q])

    def group_start(group, send, recv):
        ref = group.at[rows(f)]
        for k in range(1, half):
            to = lax.rem(f + 2 * k, F)
            remote(ref, ref, send.at[k], recv.at[f], {"fs": to}).start()
        remote(ref, ref, send.at[0], recv.at[f], {"fs": partner}).start()

    def group_forward(group, send, recv):
        for k in range(1, half):
            source = lax.rem(f - 2 * k + F, F)
            ref = group.at[rows(source)]
            landed(ref, recv.at[source])
            remote(ref, ref, send.at[half - 1 + k], recv.at[source], {"fs": partner}).start()

    def forwards_landed(group, recv):
        for k in range(1, half):
            source = lax.rem(partner + 2 * k, F)
            landed(group.at[rows(source)], recv.at[source])

    def group_sent(group, send):
        for k in range(F - 1):
            left_for(group.at[rows(f)], send.at[k])

    scale = down_scale[:, pl.ds(pl.multiple_of(z * d, d), d)]
    scaled = (cotangent[...].astype(F32) * scale).astype(BF16)
    for g in range(chunks):
        blocks[0, z, g] = scaled[:, g * cw:(g + 1) * cw]
    positive = jnp.maximum(pre_act[...].astype(F32), 0.0)
    act_group[rows(f), :] = (positive * positive).astype(BF16)
    pl.semaphore_wait(barrier, F * T - 1 + reps - 1)
    own_block(0)
    group_start(act_group, act_send, act_recv)
    for g in range(chunks):
        blocks[1, z, g] = acts[:, g * cw:(g + 1) * cw]
    down_load.wait()
    down_bf[...] = down_f32[...].astype(BF16)
    for s in range(1, T):
        if s == T - 1:
            group_forward(act_group, act_send, act_recv)
        arriving(0, s)
    own_block(1)

    def partial_of(target, e):
        value = jnp.zeros((n, hp), F32)
        for q in range(per):
            value = value + dot(
                scaled_cols[q, rows(target), :],
                down_bf[e * hp:(e + 1) * hp, q * cw:(q + 1) * cw], ((1,), (1,)),
            )
        return value

    for e in range(parts):
        def for_partner(k, carry):
            i = lax.rem(place + k, half)
            if e == 0:
                cols_landed(0, 2 * i + 1 - core)
            pair_out[e, i] = partial_of(2 * i + 1 - core, e).astype(BF16)
            remote(
                pair_out.at[e, i], pair_in.at[e, i], pair_send.at[e, i], pair_recv.at[e, i],
                {"fs": partner},
            ).start()
            return carry

        lax.fori_loop(1, half + 1, for_partner, 0)
    for e in range(parts):
        def for_far(k, carry):
            i = lax.rem(place + k, half)
            if e == 0:
                cols_landed(0, 2 * i + core)
            value = partial_of(2 * i + core, e)
            landed(pair_in.at[e, i], pair_recv.at[e, i])
            far_out[e, i] = (value + pair_in[e, i].astype(F32)).astype(BF16)
            remote(
                far_out.at[e, i], far_in.at[e, place], far_send.at[e, i], far_recv.at[e, place],
                {"fs": 2 * i + core},
            ).start()
            return carry

        lax.fori_loop(1, half, for_far, 0)
    for e in range(parts):
        value = partial_of(f, e)
        landed(pair_in.at[e, place], pair_recv.at[e, place])
        d_act[e] = value + pair_in[e, place].astype(F32)

    landed(act_group.at[rows(partner)], act_recv.at[partner])
    forwards_landed(act_group, act_recv)
    gd_rows = gd_out.shape[1]

    def rep_copy(out, into, send, recv, c, p):
        to = lax.rem(r + p, reps)
        return remote(
            out.at[c], into.at[p - 1, c], send.at[p - 1, c], recv.at[p - 1, c], {"rep": to}
        )

    def down_step(c, carry):
        at = pl.ds(pl.multiple_of(c * gd_rows, gd_rows), gd_rows)
        for q in range(per):
            value = dot(act_group[:, at], scaled_cols[q], ((0,), (0,))) * norm_factor
            gd_out[c, :, q * cw:(q + 1) * cw] = value.astype(BF16)
        for p in range(1, reps):
            rep_copy(gd_out, gd_in, gd_send, gd_recv, c, p).start()
        return carry

    lax.fori_loop(0, gd_out.shape[0], down_step, 0)
    arriving(1, 1)
    for e in range(parts):
        total = d_act[e]
        for k in range(1, half):
            j = lax.rem(place + k, half)
            landed(far_in.at[e, j], far_recv.at[e, j])
            total = total + far_in[e, j].astype(F32)
        at = slice(e * hp, (e + 1) * hp)
        positive = jnp.maximum(pre_act[:, at].astype(F32), 0.0)
        dpre_group[e, rows(f), :] = (2.0 * positive * total * up_scale[:, at]).astype(BF16)
        group_start(dpre_group.at[e], dpre_send.at[e], dpre_recv.at[e])
        if e == 0:
            up_load.wait()
            up_bf[...] = up_f32[...].astype(BF16)
            for s in range(2, T - 1):
                arriving(1, s)
    if T > 2:
        arriving(1, T - 1)

    def send_home(ref, source):
        home, slot = lax.div(source, sub), z * sub + lax.rem(source, sub)

        @pl.when(home != z)
        def _():
            remote(
                ref, gi_in.at[slot], gi_send.at[source], gi_recv.at[slot], {"tp": home}
            ).start()

        @pl.when(home == z)
        def _():
            gi_in[slot] = ref[...]

    def input_part(source):
        value = jnp.zeros((n, w), F32)
        for e in range(parts):
            value = value + dot(
                dpre_group[e, rows(source), :], up_bf[:, e * hp:(e + 1) * hp], ((1,), (1,))
            )
        gi_out[source] = value.astype(BF16)

        if source is f:
            send_home(gi_out.at[source], f)
        else:
            remote(
                gi_out.at[source], gi_mid.at[f], mid_send.at[source], mid_recv.at[f],
                {"fs": source},
            ).start()

    def relay(source):
        landed(gi_mid.at[source], mid_recv.at[source])
        send_home(gi_mid.at[source], source)

    input_part(f)
    for e in range(parts):
        landed(dpre_group.at[e, rows(partner)], dpre_recv.at[e, partner])
    input_part(partner)
    relay(partner)

    def up_step(e):
        forwards_landed(dpre_group.at[e], dpre_recv.at[e])
        for q in range(per):
            value = dot(acts_cols[q], dpre_group[e], ((0,), (0,)))
            gu_out[e, q * cw:(q + 1) * cw, :] = (value * norm_factor).astype(BF16)
        for p in range(1, reps):
            rep_copy(gu_out, gu_in, gu_send, gu_recv, e, p).start()

    for e in range(parts):
        group_forward(dpre_group.at[e], dpre_send.at[e], dpre_recv.at[e])
        if e == 0:
            for source in range(F):
                cols_landed(1, source)
        if e < parts - 1:
            up_step(e)
    for k in range(1, half):
        input_part(lax.rem(f + 2 * k, F))
    forwards_landed(dpre_group.at[parts - 1], dpre_recv.at[parts - 1])
    for k in range(1, half):
        input_part(lax.rem(partner + 2 * k, F))
    for q in range(per):
        value = dot(acts_cols[q], dpre_group[parts - 1], ((0,), (0,)))
        gu_out[parts - 1, q * cw:(q + 1) * cw, :] = (value * norm_factor).astype(BF16)
    for p in range(1, reps):
        rep_copy(gu_out, gu_in, gu_send, gu_recv, parts - 1, p).start()
    for k in range(1, half):
        relay(lax.rem(f + 2 * k, F))
        relay(lax.rem(partner + 2 * k, F))

    def total_of(out, into, send, recv, c):
        for p in range(1, reps):
            rep_copy(out, into, send, recv, c, p).wait()
        value = out[c].astype(F32)
        for p in range(1, reps):
            value = value + into[p - 1, c].astype(F32)
        return value

    def finish_down(c, carry):
        at = pl.ds(pl.multiple_of(c * gd_rows, gd_rows), gd_rows)
        grad_down[at, :] = total_of(gd_out, gd_in, gd_send, gd_recv, c)
        return carry

    lax.fori_loop(0, gd_out.shape[0], finish_down, 0)
    for e in range(parts - 1):
        grad_up[:, e * hp:(e + 1) * hp] = total_of(gu_out, gu_in, gu_send, gu_recv, e)
    for j in range(sub):
        value = jnp.zeros((n, w), F32)
        for s in range(T):
            at = s * sub + j

            @pl.when(s != z)
            def _():
                landed(gi_in.at[at], gi_recv.at[at])

            value = value + gi_in[at].astype(F32)
        grad_input[:, j * w:(j + 1) * w] = value.astype(BF16)
    grad_up[:, (parts - 1) * hp:] = total_of(gu_out, gu_in, gu_send, gu_recv, parts - 1)

    for a in range(2):
        for block in range(T):
            for g in range(chunks):
                @pl.when((block <= z) & (z < T - 1))
                def _():
                    left_for(blocks.at[a, block, g], z_send.at[a, block, g, 0])

                @pl.when((block >= z) & (z > 0))
                def _():
                    left_for(blocks.at[a, block, g], z_send.at[a, block, g, 1])

                @pl.when(block * sub + g // per != f)
                def _():
                    left_for(blocks.at[a, block, g], col_send.at[a, block, g])
    group_sent(act_group, act_send)
    for e in range(parts):
        group_sent(dpre_group.at[e], dpre_send.at[e])
        for i in range(half):
            left_for(pair_out.at[e, i], pair_send.at[e, i])

            @pl.when(i != place)
            def _():
                left_for(far_out.at[e, i], far_send.at[e, i])
    for source in range(F):
        @pl.when(source != f)
        def _():
            left_for(gi_out.at[source], mid_send.at[source])

        @pl.when(source // sub != z)
        def _():
            left_for(gi_mid.at[source], gi_send.at[source])


def body(sizes, acts, cotangent, pre_act, up_store, up_scale, down_store, down_scale):
    reps, F, T = sizes
    n, d = acts.shape
    h = pre_act.shape[1]
    w = down_store.shape[1]
    half = F // 2
    cw = w // 2 if w % 256 == 0 else w
    per, chunks = w // cw, d // cw
    parts = 2 if h % 256 == 0 else 1
    hp = h // parts
    gd_rows = fitting(h, 256)
    gd_steps = h // gd_rows
    others = max(reps - 1, 1)
    sem = pltpu.SemaphoreType.DMA
    vmem, anywhere = (pl.BlockSpec(memory_space=s) for s in (pltpu.VMEM, pltpu.HBM))
    arrays = [
        ((w, h), F32), ((h, w), F32),
        ((2, T, chunks, n, cw), BF16),
        ((per, F * n, cw), BF16), ((per, F * n, cw), BF16),
        ((F * n, h), BF16), ((parts, F * n, hp), BF16),
        ((h, w), BF16), ((w, h), BF16),
        ((parts, half, n, hp), BF16), ((parts, half, n, hp), BF16),
        ((parts, half, n, hp), BF16), ((parts, half, n, hp), BF16),
        ((parts, n, hp), F32),
        ((F, n, w), BF16), ((F, n, w), BF16), ((F, n, w), BF16),
        ((gd_steps, gd_rows, w), BF16), ((others, gd_steps, gd_rows, w), BF16),
        ((parts, w, hp), BF16), ((others, parts, w, hp), BF16),
    ]
    return pl.pallas_call(
        functools.partial(kernel, sizes),
        out_shape=(
            jax.ShapeDtypeStruct((n, d), BF16),
            jax.ShapeDtypeStruct((w, h), F32),
            jax.ShapeDtypeStruct((h, w), F32),
        ),
        in_specs=[vmem, vmem, vmem, anywhere, vmem, anywhere, vmem],
        out_specs=(vmem, vmem, vmem),
        scratch_shapes=[pltpu.VMEM(shape, kind) for shape, kind in arrays] + [
            sem((2,)),
            sem((2, T, chunks, 2)), sem((2, T, chunks)), sem((2, T, chunks)), sem((2, F, per)),
            sem((F,)), sem((F,)), sem((parts, F)), sem((parts, F)),
            sem((parts, half)), sem((parts, half)), sem((parts, half)), sem((parts, half)),
            sem((F,)), sem((F,)), sem((F,)), sem((F,)),
            sem((others, gd_steps)), sem((others, gd_steps)),
            sem((others, parts)), sem((others, parts)),
        ],
        compiler_params=pltpu.CompilerParams(
            collective_id=0, has_side_effects=True,
            vmem_limit_bytes=60 * 1024 * 1024,
        ),
    )(
        acts, cotangent, pre_act, up_store, up_scale.reshape(1, h), down_store,
        down_scale.reshape(1, d * T),
    )


def solution(mesh):
    sizes = (mesh.shape["rep"], mesh.shape["fs"], mesh.shape["tp"])
    return jax.shard_map(
        functools.partial(body, sizes),
        mesh=mesh,
        in_specs=(
            P(("rep", "fs"), "tp"),
            P(("rep", "fs"), "tp"),
            P(("rep", "fs"), "tp"),
            P("fs", "tp"),
            P("tp"),
            P("tp", "fs"),
            P(),
        ),
        out_specs=(P(("rep", "fs"), "tp"), P("fs", "tp"), P("tp", "fs")),
        check_vma=False,
    )
```
